32 devices in a mesh: kv: 16 (over z, y, x), tp: 2 (over core).
Axes of the slice: x: 2, y: 2, z: 4, core: 2. Of those that a mesh axis runs over, the one named last changes fastest.
Arguments:
- residual_in: bfloat16 [96, 2048], P('kv', 'tp'), may hold values from -36 to 36
- gain_pre: float32 [2048], P('tp'), may hold values from 0.1 to 1.9
- gate_pre: bfloat16 [2048, 5632], P('tp', 'kv'), may hold values from -0.125 to 0.125
- up_pre: bfloat16 [2048, 5632], P('tp', 'kv'), may hold values from -0.125 to 0.125
- down_pre: bfloat16 [5632, 2048], P('kv', 'tp'), may hold values from -0.078125 to 0.078125
- gain_mix: float32 [2048], replicated, may hold values from 0.1 to 1.9
- query_weight: bfloat16 [2048, 2048], P('kv', 'tp'), may hold values from -0.125 to 0.125
- forget_weight: bfloat16 [2048, 2048], P('kv', 'tp'), may hold values from -0.125 to 0.125
- value_weight: bfloat16 [2048, 2048], P('kv', 'tp'), may hold values from -0.125 to 0.125
- outgate_weight: bfloat16 [2048, 2048], P('kv', 'tp'), may hold values from -0.125 to 0.125
- lower_bound: float32 [2048], P('tp'), may hold values from 0.05 to 0.95
- head_gain: float32 [2048], P('tp'), may hold values from 0.1 to 1.9
- out_weight: bfloat16 [2048, 2048], P('tp'), may hold values from -0.125 to 0.125
- gain_post: float32 [2048], P('tp'), may hold values from 0.1 to 1.9
- gate_post: bfloat16 [2048, 5632], P('tp', 'kv'), may hold values from -0.125 to 0.125
- up_post: bfloat16 [2048, 5632], P('tp', 'kv'), may hold values from -0.125 to 0.125
- down_post: bfloat16 [5632, 2048], P('kv', 'tp'), may hold values from -0.078125 to 0.078125
- memory_state: float32 [96, 16, 128, 128], P('kv', 'tp'), may hold values from -4 to 4
Outputs:
- layer_out: bfloat16 [96, 2048], P('kv', 'tp')
- next_state: float32 [96, 16, 128, 128], P('kv', 'tp')
The draws below stay inside these ranges and needn't reach their ends.
All inputs are finite; a program needn't handle non-finite values.
Results may differ from the reference program's by a relative error of at most 0.014.
Values may be sent and summed in bfloat16 or wider, within the bound.
A program may use at most 64 MiB of HBM per device.

```python
import math
import jax
import jax.numpy as jnp
from jax import lax

D = 2048
FF = 5632
HEADS = 16
HEAD_DIM = 128
HW = 2048
BATCH = 96


def draw_residual_in(key, part):
    key_base = jax.random.fold_in(key, 11)
    key_cols = jax.random.fold_in(key, 12)
    key_rows = jax.random.fold_in(key, 13)
    column_pos = jnp.arange(D, dtype=jnp.float32) / D
    col_scale = 4.0 ** column_pos * jax.random.uniform(key_cols, (D,), jnp.float32, 0.5, 1.5)
    row_scale = jnp.exp(jax.random.uniform(key_rows, (BATCH, 1), jnp.float32, 0.0, math.log(10.0)))
    base_vals = jnp.clip(jax.random.normal(key_base, (BATCH, D), jnp.float32), -4.0, 4.0)
    return (0.15 * base_vals * col_scale[None, :] * row_scale).astype(jnp.bfloat16)


def block_scale(key, dims, split, smallest, high):
    factor_of = 1.0
    for dim, shards_of in split:
        heights = jax.random.uniform(jax.random.fold_in(jax.random.fold_in(key, 6), dim), (shards_of,), jnp.float32, smallest / len(split), high / len(split))
        factor_of = factor_of * jnp.repeat(jnp.exp(heights), dims[dim] // shards_of).reshape((-1,) + (1,) * (len(dims) - 1 - dim))
    return factor_of


def bell_draw(rng, extent, scale, reach, cuts=(), kind=jnp.bfloat16):
    array = scale * jax.random.normal(rng, extent, jnp.float32)
    if cuts:
        array = array * block_scale(rng, extent, cuts, -0.22, 0.18)
    return jnp.clip(array, -reach, reach).astype(kind)


def setup_inputs(seed: int = 0) -> dict:
    key_of = jax.random.split(jax.random.key(seed), 19)
    residual_in = draw_residual_in(jax.random.fold_in(key_of[18], 71), 0)
    gain_pre = jnp.clip(1.0 + 0.18 * jax.random.normal(key_of[1], (D,), jnp.float32), 0.1, 1.9)
    gate_pre = bell_draw(key_of[2], (D, FF), D ** -0.5, 0.125, ((0, 2), (1, 16)))
    up_pre = bell_draw(key_of[3], (D, FF), D ** -0.5, 0.125, ((0, 2), (1, 16)))
    down_pre = bell_draw(key_of[4], (FF, D), FF ** -0.5, 0.078125, ((0, 16), (1, 2)))
    gain_mix = jnp.clip(1.0 + 0.18 * jax.random.normal(key_of[5], (D,), jnp.float32), 0.1, 1.9)
    query_weight = bell_draw(key_of[6], (D, HW), D ** -0.5, 0.125, ((0, 16), (1, 2)))
    forget_weight = bell_draw(key_of[7], (D, HW), D ** -0.5, 0.125, ((0, 16), (1, 2)))
    value_weight = bell_draw(key_of[8], (D, HW), D ** -0.5, 0.125, ((0, 16), (1, 2)))
    outgate_weight = bell_draw(key_of[9], (D, HW), D ** -0.5, 0.125, ((0, 16), (1, 2)))
    lower_bound = jnp.clip(0.05 + 0.9 * jax.random.uniform(key_of[10], (HW,), jnp.float32) ** block_scale(key_of[10], (HW,), ((0, 2),), -0.2, 0.2), 0.05, 0.95)
    head_gain = jnp.clip(1.0 + 0.18 * jax.random.normal(key_of[11], (HW,), jnp.float32), 0.1, 1.9)
    out_weight = bell_draw(key_of[12], (HW, D), HW ** -0.5, 0.125, ((0, 2),))
    gain_post = jnp.clip(1.0 + 0.18 * jax.random.normal(key_of[13], (D,), jnp.float32), 0.1, 1.9)
    gate_post = bell_draw(key_of[14], (D, FF), D ** -0.5, 0.125, ((0, 2), (1, 16)))
    up_post = bell_draw(key_of[15], (D, FF), D ** -0.5, 0.125, ((0, 2), (1, 16)))
    down_post = bell_draw(key_of[16], (FF, D), FF ** -0.5, 0.078125, ((0, 16), (1, 2)))
    memory_state = bell_draw(key_of[17], (BATCH, HEADS, HEAD_DIM, HEAD_DIM), 0.5, 4.0, ((0, 16), (1, 2)), jnp.float32)
    return dict(residual_in=residual_in, gain_pre=gain_pre, gate_pre=gate_pre, up_pre=up_pre, down_pre=down_pre, gain_mix=gain_mix, query_weight=query_weight, forget_weight=forget_weight, value_weight=value_weight, outgate_weight=outgate_weight, lower_bound=lower_bound, head_gain=head_gain, out_weight=out_weight, gain_post=gain_post, gate_post=gate_post, up_post=up_post, down_post=down_post, memory_state=memory_state)


EPSILON = 1e-06

def channel_mixer(stream, gain_vec, gate_weight, up_weight, down_weight):
    widened = stream.astype(jnp.float32)
    inverse = lax.rsqrt(lax.optimization_barrier(jnp.mean(widened * widened, axis=1, keepdims=True)) + EPSILON)
    scaled = (widened * gain_vec).astype(jnp.bfloat16)
    gate_sum = jnp.dot(scaled, gate_weight, preferred_element_type=jnp.float32) * inverse
    up_sum = jnp.dot(scaled, up_weight, preferred_element_type=jnp.float32) * inverse
    hidden = (jax.nn.silu(gate_sum) * up_sum).astype(jnp.bfloat16)
    return jnp.dot(hidden, down_weight, preferred_element_type=jnp.float32)

def token_mixer(stream, gain_mix, query_weight, forget_weight, value_weight, outgate_weight, lower_bound, head_gain, out_weight, memory_state):
    widened = stream.astype(jnp.float32)
    inverse = lax.rsqrt(lax.optimization_barrier(jnp.mean(widened * widened, axis=1, keepdims=True)) + EPSILON)
    scaled = (widened * gain_mix).astype(jnp.bfloat16)
    batch_rows = stream.shape[0]

    def project(weight_mat):
        product = jnp.dot(scaled, weight_mat, preferred_element_type=jnp.float32) * inverse
        return product.reshape(batch_rows, HEADS, HEAD_DIM)
    query_pre = project(query_weight)
    forget_pre = project(forget_weight)
    value_pre = project(value_weight)
    outgate_pre = project(outgate_weight)
    floor_rate = lower_bound.reshape(HEADS, HEAD_DIM)
    log_keep = jnp.logaddexp(jnp.log(floor_rate), jnp.log1p(-floor_rate) + jax.nn.log_sigmoid(forget_pre))
    inject = (1.0 - floor_rate) * jax.nn.sigmoid(-forget_pre)
    next_state = jnp.exp(log_keep)[..., None] * memory_state + inject[..., None] * value_pre[:, :, None, :]
    readout = jnp.einsum('bhk,bhkv->bhv', jax.nn.silu(query_pre), next_state, precision=lax.Precision.HIGHEST)
    normed = readout * lax.rsqrt(lax.optimization_barrier(jnp.mean(readout * readout, axis=2, keepdims=True)) + EPSILON) * head_gain.reshape(HEADS, HEAD_DIM)
    mixed_heads = (normed * jax.nn.silu(outgate_pre)).reshape(batch_rows, HEADS * HEAD_DIM).astype(jnp.bfloat16)
    mixed = jnp.dot(mixed_heads, out_weight, preferred_element_type=jnp.float32)
    return (mixed, next_state)

def reference(residual_in, gain_pre, gate_pre, up_pre, down_pre, gain_mix, query_weight, forget_weight, value_weight, outgate_weight, lower_bound, head_gain, out_weight, gain_post, gate_post, up_post, down_post, memory_state):
    branch_a = channel_mixer(residual_in, gain_pre, gate_pre, up_pre, down_pre)
    stream_a = (residual_in.astype(jnp.float32) + 0.5 * branch_a).astype(jnp.bfloat16)
    mixed, next_state = token_mixer(stream_a, gain_mix, query_weight, forget_weight, value_weight, outgate_weight, lower_bound, head_gain, out_weight, memory_state)
    stream_b = (stream_a.astype(jnp.float32) + mixed).astype(jnp.bfloat16)
    branch_b = channel_mixer(stream_b, gain_post, gate_post, up_post, down_post)
    layer_out = (stream_b.astype(jnp.float32) + 0.5 * branch_b).astype(jnp.bfloat16)
    return (layer_out, next_state)
```

```python
import functools

import jax
import jax.numpy as jnp
from jax import lax
from jax.experimental import pallas as pl
from jax.experimental.pallas import tpu as pltpu
from jax.sharding import PartitionSpec as P

D = 2048
HEAD_DIM = 128


EPSILON = 1e-06


def channel_mixer(row_block, gain_vec, gate_weight, up_weight, down_weight):
    gathered = lax.all_gather(row_block, "kv", axis=0, tiled=True)
    widened = gathered.astype(jnp.float32)
    part_squares = jnp.sum(widened * widened, axis=1)
    scaled = (widened * gain_vec).astype(jnp.bfloat16)
    gate_part = jnp.dot(scaled, gate_weight, preferred_element_type=jnp.float32)
    up_part = jnp.dot(scaled, up_weight, preferred_element_type=jnp.float32)
    gate_share, up_share, square_share = (
        lax.psum_scatter(
            gate_part.astype(jnp.bfloat16), "tp", scatter_dimension=0, tiled=True
        ).astype(jnp.float32),
        lax.psum_scatter(
            up_part.astype(jnp.bfloat16), "tp", scatter_dimension=0, tiled=True
        ).astype(jnp.float32),
        lax.psum_scatter(
            part_squares.astype(jnp.bfloat16), "tp", scatter_dimension=0, tiled=True
        ).astype(jnp.float32),
    )
    share_inverse = lax.rsqrt(square_share / D + EPSILON)[:, None]
    hidden_share = (jax.nn.silu(gate_share * share_inverse) * (up_share * share_inverse)).astype(
        jnp.bfloat16
    )
    hidden = lax.all_gather(hidden_share, "tp", axis=0, tiled=True)
    return lax.psum_scatter(
        jnp.dot(hidden, down_weight, preferred_element_type=jnp.float32),
        "kv",
        scatter_dimension=0,
        tiled=True,
    )


def token_mixer(
    stream_a,
    gain_mix,
    query_weight,
    forget_weight,
    value_weight,
    outgate_weight,
    lower_bound,
    head_gain,
    out_weight,
    memory_state,
):
    full_rows = lax.all_gather(stream_a, "tp", axis=1, tiled=True)
    widened = full_rows.astype(jnp.float32)
    inverse = lax.rsqrt(jnp.mean(widened * widened, axis=1, keepdims=True) + EPSILON)
    scaled = (widened * gain_mix).astype(jnp.bfloat16)
    weights = (query_weight, forget_weight, value_weight, outgate_weight)
    blocks = lax.all_to_all(scaled, "kv", split_axis=1, concat_axis=0, tiled=True)
    joined = jnp.concatenate(weights, axis=1)
    projected = lax.psum_scatter(
        jnp.dot(blocks, joined, preferred_element_type=jnp.float32),
        "kv",
        scatter_dimension=0,
        tiled=True,
    )
    projected = projected * inverse
    seq_rows = scaled.shape[0]
    local_heads = query_weight.shape[1] // HEAD_DIM
    reshaped = projected.reshape(seq_rows, 4, local_heads, HEAD_DIM)
    query_pre = reshaped[:, 0]
    forget_pre = reshaped[:, 1]
    value_pre = reshaped[:, 2]
    outgate_pre = reshaped[:, 3]
    floor_rate = lower_bound.reshape(local_heads, HEAD_DIM)
    log_keep = jnp.logaddexp(
        jnp.log(floor_rate), jnp.log1p(-floor_rate) + jax.nn.log_sigmoid(forget_pre)
    )
    inject = (1.0 - floor_rate) * jax.nn.sigmoid(-forget_pre)
    next_state = (
        jnp.exp(log_keep)[..., None] * memory_state + inject[..., None] * value_pre[:, :, None, :]
    )
    readout = jnp.einsum(
        "bhk,bhkv->bhv", jax.nn.silu(query_pre), next_state, precision=lax.Precision.HIGHEST
    )
    normed = (
        readout
        * lax.rsqrt(jnp.mean(readout * readout, axis=2, keepdims=True) + EPSILON)
        * head_gain.reshape(local_heads, HEAD_DIM)
    )
    mixed_heads = (
        (normed * jax.nn.silu(outgate_pre))
        .reshape(seq_rows, local_heads * HEAD_DIM)
        .astype(jnp.bfloat16)
    )
    partial_out = jnp.dot(mixed_heads, out_weight, preferred_element_type=jnp.float32)
    mixed = lax.psum_scatter(
        partial_out.astype(jnp.bfloat16), "tp", scatter_dimension=1, tiled=True
    ).astype(jnp.float32)
    return (mixed, next_state)


def shards(
    residual_in,
    gain_pre,
    gate_pre,
    up_pre,
    down_pre,
    gain_mix,
    query_weight,
    forget_weight,
    value_weight,
    outgate_weight,
    lower_bound,
    head_gain,
    out_weight,
    gain_post,
    gate_post,
    up_post,
    down_post,
    memory_state,
):
    branch_a = channel_mixer(residual_in, gain_pre, gate_pre, up_pre, down_pre)
    stream_a = (residual_in.astype(jnp.float32) + 0.5 * branch_a).astype(jnp.bfloat16)
    mixed, next_state = token_mixer(
        stream_a,
        gain_mix,
        query_weight,
        forget_weight,
        value_weight,
        outgate_weight,
        lower_bound,
        head_gain,
        out_weight,
        memory_state,
    )
    stream_b = (stream_a.astype(jnp.float32) + mixed).astype(jnp.bfloat16)
    branch_b = channel_mixer(stream_b, gain_post, gate_post, up_post, down_post)
    layer_out = (stream_b.astype(jnp.float32) + 0.5 * branch_b).astype(jnp.bfloat16)
    return (layer_out, next_state)


ROW_PAD = 8
GATHER_A, SCATTER_A, COLUMNS, PROJECT, GATHER_B, SCATTER_B = 0, 1, 2, 3, 7, 8
KV_EXCHANGES = 9


def fused_layer(
    n_kv,
    residual_ref,
    gain_pre_ref,
    gain_mix_ref,
    lower_ref,
    head_gain_ref,
    gain_post_ref,
    gate_pre_hbm,
    up_pre_hbm,
    down_pre_hbm,
    query_hbm,
    forget_hbm,
    value_hbm,
    outgate_hbm,
    out_hbm,
    gate_post_hbm,
    up_post_hbm,
    down_post_hbm,
    state_hbm,
    layer_ref,
    next_hbm,
    gate_pre,
    up_pre,
    down_pre,
    proj_weights,
    out_weight,
    gate_post,
    up_post,
    down_post,
    state,
    gather_a,
    gather_b,
    partial_a,
    partial_b,
    landed_a,
    landed_b,
    gate_up_out,
    gate_up_in,
    squares_out,
    squares_in,
    stream_out,
    stream_in,
    column_out,
    column_in,
    proj_out,
    proj_in,
    mixed_out,
    mixed_in,
    residual_pad,
    keep_t,
    inject_t,
    query_t,
    value_rows,
    readout,
    load_sem,
    store_sem,
    kv_send,
    kv_recv,
    tp_send,
    tp_recv,
):
    me = lax.axis_index("kv")
    core = lax.axis_index("tp")
    rows, width = residual_ref.shape
    model = 2 * width
    f32, bf16 = jnp.float32, jnp.bfloat16

    def load(index, source, target):
        return pltpu.make_async_copy(source, target, load_sem.at[index])

    loads = [
        load(0, gate_pre_hbm, gate_pre),
        load(1, up_pre_hbm, up_pre),
        load(2, down_pre_hbm, down_pre),
        load(3, forget_hbm, proj_weights.at[0]),
        load(4, value_hbm, proj_weights.at[1]),
        load(5, query_hbm, proj_weights.at[2]),
        load(6, outgate_hbm, proj_weights.at[3]),
        load(7, state_hbm, state),
        load(8, out_hbm, out_weight),
        load(9, gate_post_hbm, gate_post),
        load(10, up_post_hbm, up_post),
        load(11, down_post_hbm, down_post),
    ]
    for copy in loads:
        copy.start()

    residual_pad[...] = jnp.zeros_like(residual_pad)
    residual_pad[0:rows, :] = residual_ref[...].astype(f32)
    gather_a[me] = residual_pad[...].astype(bf16)
    readout[...] = jnp.zeros_like(readout)

    barrier = pltpu.get_barrier_semaphore()

    def greet(step, carry):
        pl.semaphore_signal(
            barrier,
            inc=1,
            device_id={"kv": lax.rem(me + step, n_kv)},
            device_id_type=pl.DeviceIdType.MESH,
        )
        return carry

    lax.fori_loop(1, n_kv, greet, 0)
    pl.semaphore_signal(
        barrier, inc=1, device_id={"tp": 1 - core}, device_id_type=pl.DeviceIdType.MESH
    )
    pl.semaphore_wait(barrier, n_kv)

    def kv_copy(exchange, source, target, peer, slot):
        return pltpu.make_async_remote_copy(
            src_ref=source,
            dst_ref=target,
            send_sem=kv_send.at[exchange, peer],
            recv_sem=kv_recv.at[exchange, slot],
            device_id={"kv": peer},
            device_id_type=pl.DeviceIdType.MESH,
        )

    def kv_start(exchange, source_of, target):
        def body(step, carry):
            peer = lax.rem(me + step, n_kv)
            kv_copy(exchange, source_of(peer), target.at[me], peer, me).start()
            return carry

        lax.fori_loop(1, n_kv, body, 0)

    def kv_arrive(exchange, target):
        def body(step, carry):
            peer = lax.rem(me + step, n_kv)
            kv_copy(exchange, target.at[peer], target.at[peer], peer, peer).wait_recv()
            return carry

        lax.fori_loop(1, n_kv, body, 0)

    def kv_sent(exchange, source_of, target):
        def body(step, carry):
            peer = lax.rem(me + step, n_kv)
            kv_copy(exchange, source_of(peer), target.at[me], peer, me).wait_send()
            return carry

        lax.fori_loop(1, n_kv, body, 0)

    def tp_copy(index, source, target):
        return pltpu.make_async_remote_copy(
            src_ref=source,
            dst_ref=target,
            send_sem=tp_send.at[index],
            recv_sem=tp_recv.at[index],
            device_id={"tp": 1 - core},
            device_id_type=pl.DeviceIdType.MESH,
        )

    def feed_forward(which, gathered, gain_ref, gate, up, down, partial, landed):
        gather_id, scatter_id = ((GATHER_A, SCATTER_A), (GATHER_B, SCATTER_B))[which]
        kv_start(gather_id, lambda peer: gathered.at[me], gathered)
        for copy in (loads[0:2], loads[9:11])[which]:
            copy.wait()
        kv_arrive(gather_id, gathered)
        wide = gathered[...].astype(f32).reshape(n_kv * ROW_PAD, width)
        squares = jnp.sum(wide * wide, axis=1, keepdims=True)
        squares_out[which] = jnp.broadcast_to(squares, squares_out.shape[1:])
        scaled = (wide * gain_ref[...]).astype(bf16)
        gate_part = jnp.dot(scaled, gate[...], preferred_element_type=f32)
        gate_up_out[which, 0] = gate_part.astype(bf16)
        copies = [
            tp_copy(3 * which, squares_out.at[which], squares_in.at[which]),
            tp_copy(3 * which + 1, gate_up_out.at[which, 0], gate_up_in.at[which, 0]),
            tp_copy(3 * which + 2, gate_up_out.at[which, 1], gate_up_in.at[which, 1]),
        ]
        copies[0].start()
        copies[1].start()
        up_part = jnp.dot(scaled, up[...], preferred_element_type=f32)
        gate_up_out[which, 1] = up_part.astype(bf16)
        copies[2].start()
        for copy in copies:
            copy.wait_recv()
        total = squares + squares_in[which][:, 0:1]
        inverse = lax.rsqrt(total / model + EPSILON)
        gate_sum = (gate_part + gate_up_in[which, 0].astype(f32)) * inverse
        up_sum = (up_part + gate_up_in[which, 1].astype(f32)) * inverse
        hidden = (gate_sum / (1.0 + jnp.exp(-gate_sum)) * up_sum).astype(bf16)
        loads[(2, 11)[which]].wait()
        branch = jnp.dot(hidden, down[...], preferred_element_type=f32)
        partial[...] = branch.reshape(n_kv, ROW_PAD, width).astype(bf16)
        landed[me] = partial[me]
        kv_start(scatter_id, lambda peer: partial.at[peer], landed)
        kv_arrive(scatter_id, landed)
        for copy in copies:
            copy.wait_send()
        return jnp.sum(landed[...].astype(f32), axis=0)

    branch_a = feed_forward(
        0, gather_a, gain_pre_ref, gate_pre, up_pre, down_pre, partial_a, landed_a
    )
    stream_a = (residual_pad[...] + 0.5 * branch_a).astype(bf16)

    stream_out[...] = stream_a
    stream_copy = tp_copy(6, stream_out, stream_in)
    stream_copy.start()
    own = stream_a.astype(f32)
    own_squares = jnp.sum(own * own, axis=1, keepdims=True)
    stream_copy.wait_recv()
    other = stream_in[...].astype(f32)
    squares = own_squares + jnp.sum(other * other, axis=1, keepdims=True)
    inverse = lax.rsqrt(squares / model + EPSILON)
    own_scaled = (own * gain_mix_ref[core]).astype(bf16)
    other_scaled = (other * gain_mix_ref[1 - core]).astype(bf16)
    depth = column_out.shape[2]
    half_blocks = n_kv // 2
    for block in range(half_blocks):
        span = slice(block * depth, (block + 1) * depth)
        column_out[core * half_blocks + block] = own_scaled[:, span]
        column_out[(1 - core) * half_blocks + block] = other_scaled[:, span]
    column_in[me] = column_out[me]
    kv_start(COLUMNS, lambda peer: column_out.at[peer], column_in)
    kv_arrive(COLUMNS, column_in)
    columns = column_in[...].astype(f32).reshape(n_kv * ROW_PAD, depth).astype(bf16)
    for index in range(4):
        loads[3 + index].wait()
        product = jnp.dot(columns, proj_weights[index], preferred_element_type=f32)
        proj_out[index] = product.reshape(n_kv, ROW_PAD, width).astype(bf16)
        proj_in[index, me] = proj_out[index, me]
        kv_start(
            PROJECT + index,
            lambda peer, index=index: proj_out.at[index, peer],
            proj_in.at[index],
        )

    def projected(index):
        kv_arrive(PROJECT + index, proj_in.at[index])
        return jnp.sum(proj_in[index].astype(f32), axis=0) * inverse

    heads = width // HEAD_DIM
    floor_rate = lower_ref[...]
    forget_pre = projected(0)
    keep = floor_rate + (1.0 - floor_rate) / (1.0 + jnp.exp(-forget_pre))
    inject = (1.0 - floor_rate) / (1.0 + jnp.exp(forget_pre))
    for head in range(heads):
        span = slice(head * HEAD_DIM, (head + 1) * HEAD_DIM)
        keep_t[head] = keep[:, span].T
        inject_t[head] = inject[:, span].T
    value_pre = projected(1)
    for head in range(heads):
        span = slice(head * HEAD_DIM, (head + 1) * HEAD_DIM)
        value_rows[head] = value_pre[:, span]
    query_pre = projected(2)
    query = query_pre / (1.0 + jnp.exp(-query_pre))
    for head in range(heads):
        span = slice(head * HEAD_DIM, (head + 1) * HEAD_DIM)
        query_t[head] = query[:, span].T
    loads[7].wait()

    def recur(head, carry):
        keep_cols = keep_t[head]
        inject_cols = inject_t[head]
        query_cols = query_t[head]
        values = value_rows[head]
        for row in range(rows):
            col = slice(row, row + 1)
            new = keep_cols[:, col] * state[row, head] + inject_cols[:, col] * values[col, :]
            state[row, head] = new
            readout[head, col, :] = jnp.sum(query_cols[:, col] * new, axis=0, keepdims=True)
        return carry

    lax.fori_loop(0, heads, recur, 0)
    store = pltpu.make_async_copy(state, next_hbm, store_sem)
    outgate_pre = projected(3)
    store.start()
    outgate = outgate_pre / (1.0 + jnp.exp(-outgate_pre))
    mixed_heads = []
    for head in range(heads):
        span = slice(head * HEAD_DIM, (head + 1) * HEAD_DIM)
        read = readout[head]
        scale = lax.rsqrt(jnp.mean(read * read, axis=1, keepdims=True) + EPSILON)
        mixed_heads.append(read * scale * head_gain_ref[:, span] * outgate[:, span])
    mixed_rows = jnp.concatenate(mixed_heads, axis=1).astype(bf16)
    loads[8].wait()
    mixed_part = jnp.dot(mixed_rows, out_weight[...], preferred_element_type=f32)
    mixed_out[0] = mixed_part[:, 0:width]
    mixed_out[1] = mixed_part[:, width:model]
    mixed_copy = tp_copy(7, mixed_out.at[1 - core], mixed_in)
    mixed_copy.start()
    mixed_copy.wait_recv()
    mixed = mixed_out[core] + mixed_in[...]
    stream_b = (stream_out[...].astype(f32) + mixed).astype(bf16)
    gather_b[me] = stream_b
    branch_b = feed_forward(
        1, gather_b, gain_post_ref, gate_post, up_post, down_post, partial_b, landed_b
    )
    layer_out = (gather_b[me].astype(f32) + 0.5 * branch_b).astype(bf16)
    layer_ref[...] = layer_out[0:rows, :]

    stream_copy.wait_send()
    mixed_copy.wait_send()
    kv_sent(GATHER_A, lambda peer: gather_a.at[me], gather_a)
    kv_sent(SCATTER_A, lambda peer: partial_a.at[peer], landed_a)
    kv_sent(COLUMNS, lambda peer: column_out.at[peer], column_in)
    for index in range(4):
        kv_sent(
            PROJECT + index,
            lambda peer, index=index: proj_out.at[index, peer],
            proj_in.at[index],
        )
    kv_sent(GATHER_B, lambda peer: gather_b.at[me], gather_b)
    kv_sent(SCATTER_B, lambda peer: partial_b.at[peer], landed_b)
    store.wait()


def fused_shards(
    n_kv,
    residual_in,
    gain_pre,
    gate_pre,
    up_pre,
    down_pre,
    gain_mix,
    query_weight,
    forget_weight,
    value_weight,
    outgate_weight,
    lower_bound,
    head_gain,
    out_weight,
    gain_post,
    gate_post,
    up_post,
    down_post,
    memory_state,
):
    rows, width = residual_in.shape
    depth = query_weight.shape[0]
    hidden = gate_pre.shape[1]
    heads = width // HEAD_DIM
    all_rows = n_kv * ROW_PAD
    f32, bf16 = jnp.float32, jnp.bfloat16
    vmem = pl.BlockSpec(memory_space=pltpu.VMEM)
    hbm = pl.BlockSpec(memory_space=pl.ANY)
    like = lambda array: pltpu.VMEM(array.shape, array.dtype)
    blocks = lambda: pltpu.VMEM((n_kv, ROW_PAD, width), bf16)
    return pl.pallas_call(
        functools.partial(fused_layer, n_kv),
        out_shape=(
            jax.ShapeDtypeStruct(residual_in.shape, residual_in.dtype),
            jax.ShapeDtypeStruct(memory_state.shape, memory_state.dtype),
        ),
        in_specs=[vmem] * 6 + [hbm] * 12,
        out_specs=(vmem, hbm),
        scratch_shapes=[
            like(gate_pre),
            like(up_pre),
            like(down_pre),
            pltpu.VMEM((4,) + query_weight.shape, bf16),
            like(out_weight),
            like(gate_post),
            like(up_post),
            like(down_post),
            like(memory_state),
            blocks(),
            blocks(),
            blocks(),
            blocks(),
            blocks(),
            blocks(),
            pltpu.VMEM((2, 2, all_rows, hidden), bf16),
            pltpu.VMEM((2, 2, all_rows, hidden), bf16),
            pltpu.VMEM((2, all_rows, 128), f32),
            pltpu.VMEM((2, all_rows, 128), f32),
            pltpu.VMEM((ROW_PAD, width), bf16),
            pltpu.VMEM((ROW_PAD, width), bf16),
            pltpu.VMEM((n_kv, ROW_PAD, depth), bf16),
            pltpu.VMEM((n_kv, ROW_PAD, depth), bf16),
            pltpu.VMEM((4, n_kv, ROW_PAD, width), bf16),
            pltpu.VMEM((4, n_kv, ROW_PAD, width), bf16),
            pltpu.VMEM((2, ROW_PAD, width), f32),
            pltpu.VMEM((ROW_PAD, width), f32),
            pltpu.VMEM((ROW_PAD, width), f32),
            pltpu.VMEM((heads, HEAD_DIM, ROW_PAD), f32),
            pltpu.VMEM((heads, HEAD_DIM, ROW_PAD), f32),
            pltpu.VMEM((heads, HEAD_DIM, ROW_PAD), f32),
            pltpu.VMEM((heads, ROW_PAD, HEAD_DIM), f32),
            pltpu.VMEM((heads, ROW_PAD, HEAD_DIM), f32),
            pltpu.SemaphoreType.DMA((12,)),
            pltpu.SemaphoreType.DMA,
            pltpu.SemaphoreType.DMA((KV_EXCHANGES, n_kv)),
            pltpu.SemaphoreType.DMA((KV_EXCHANGES, n_kv)),
            pltpu.SemaphoreType.DMA((8,)),
            pltpu.SemaphoreType.DMA((8,)),
        ],
        compiler_params=pltpu.CompilerParams(
            collective_id=0, has_side_effects=True, vmem_limit_bytes=60 * 1024 * 1024
        ),
    )(
        residual_in,
        gain_pre.reshape(1, width),
        gain_mix.reshape(2, 1, width),
        lower_bound.reshape(1, width),
        head_gain.reshape(1, width),
        gain_post.reshape(1, width),
        gate_pre,
        up_pre,
        down_pre,
        query_weight,
        forget_weight,
        value_weight,
        outgate_weight,
        out_weight,
        gate_post,
        up_post,
        down_post,
        memory_state,
    )


def solution(mesh):
    n_kv, n_tp = mesh.shape["kv"], mesh.shape["tp"]
    fits = n_tp == 2 and D % (128 * n_kv) == 0 and n_kv % 2 == 0
    body = functools.partial(fused_shards, n_kv) if fits else shards
    in_specs = (
        P("kv", "tp"),
        P("tp"),
        P("tp", "kv"),
        P("tp", "kv"),
        P("kv", "tp"),
        P(),
        P("kv", "tp"),
        P("kv", "tp"),
        P("kv", "tp"),
        P("kv", "tp"),
        P("tp"),
        P("tp"),
        P("tp", None),
        P("tp"),
        P("tp", "kv"),
        P("tp", "kv"),
        P("kv", "tp"),
        P("kv", "tp", None, None),
    )
    out_specs = (P("kv", "tp"), P("kv", "tp", None, None))
    return jax.shard_map(body, mesh=mesh, in_specs=in_specs, out_specs=out_specs, check_vma=False)
```

```python
import functools

import jax
import jax.numpy as jnp
from jax import lax
from jax.experimental import pallas as pl
from jax.experimental.pallas import tpu as pltpu
from jax.sharding import PartitionSpec as P

D = 2048
HEAD_DIM = 128


EPSILON = 1e-06


def channel_mixer(row_block, gain_vec, gate_weight, up_weight, down_weight):
    gathered = lax.all_gather(row_block, "kv", axis=0, tiled=True)
    widened = gathered.astype(jnp.float32)
    part_squares = jnp.sum(widened * widened, axis=1)
    scaled = (widened * gain_vec).astype(jnp.bfloat16)
    gate_part = jnp.dot(scaled, gate_weight, preferred_element_type=jnp.float32)
    up_part = jnp.dot(scaled, up_weight, preferred_element_type=jnp.float32)
    gate_share, up_share, square_share = (
        lax.psum_scatter(
            gate_part.astype(jnp.bfloat16), "tp", scatter_dimension=0, tiled=True
        ).astype(jnp.float32),
        lax.psum_scatter(
            up_part.astype(jnp.bfloat16), "tp", scatter_dimension=0, tiled=True
        ).astype(jnp.float32),
        lax.psum_scatter(
            part_squares.astype(jnp.bfloat16), "tp", scatter_dimension=0, tiled=True
        ).astype(jnp.float32),
    )
    share_inverse = lax.rsqrt(square_share / D + EPSILON)[:, None]
    hidden_share = (jax.nn.silu(gate_share * share_inverse) * (up_share * share_inverse)).astype(
        jnp.bfloat16
    )
    hidden = lax.all_gather(hidden_share, "tp", axis=0, tiled=True)
    return lax.psum_scatter(
        jnp.dot(hidden, down_weight, preferred_element_type=jnp.float32),
        "kv",
        scatter_dimension=0,
        tiled=True,
    )


def token_mixer(
    stream_a,
    gain_mix,
    query_weight,
    forget_weight,
    value_weight,
    outgate_weight,
    lower_bound,
    head_gain,
    out_weight,
    memory_state,
):
    full_rows = lax.all_gather(stream_a, "tp", axis=1, tiled=True)
    widened = full_rows.astype(jnp.float32)
    inverse = lax.rsqrt(jnp.mean(widened * widened, axis=1, keepdims=True) + EPSILON)
    scaled = (widened * gain_mix).astype(jnp.bfloat16)
    weights = (query_weight, forget_weight, value_weight, outgate_weight)
    blocks = lax.all_to_all(scaled, "kv", split_axis=1, concat_axis=0, tiled=True)
    joined = jnp.concatenate(weights, axis=1)
    projected = lax.psum_scatter(
        jnp.dot(blocks, joined, preferred_element_type=jnp.float32),
        "kv",
        scatter_dimension=0,
        tiled=True,
    )
    projected = projected * inverse
    seq_rows = scaled.shape[0]
    local_heads = query_weight.shape[1] // HEAD_DIM
    reshaped = projected.reshape(seq_rows, 4, local_heads, HEAD_DIM)
    query_pre = reshaped[:, 0]
    forget_pre = reshaped[:, 1]
    value_pre = reshaped[:, 2]
    outgate_pre = reshaped[:, 3]
    floor_rate = lower_bound.reshape(local_heads, HEAD_DIM)
    log_keep = jnp.logaddexp(
        jnp.log(floor_rate), jnp.log1p(-floor_rate) + jax.nn.log_sigmoid(forget_pre)
    )
    inject = (1.0 - floor_rate) * jax.nn.sigmoid(-forget_pre)
    next_state = (
        jnp.exp(log_keep)[..., None] * memory_state + inject[..., None] * value_pre[:, :, None, :]
    )
    readout = jnp.einsum(
        "bhk,bhkv->bhv", jax.nn.silu(query_pre), next_state, precision=lax.Precision.HIGHEST
    )
    normed = (
        readout
        * lax.rsqrt(jnp.mean(readout * readout, axis=2, keepdims=True) + EPSILON)
        * head_gain.reshape(local_heads, HEAD_DIM)
    )
    mixed_heads = (
        (normed * jax.nn.silu(outgate_pre))
        .reshape(seq_rows, local_heads * HEAD_DIM)
        .astype(jnp.bfloat16)
    )
    partial_out = jnp.dot(mixed_heads, out_weight, preferred_element_type=jnp.float32)
    mixed = lax.psum_scatter(
        partial_out.astype(jnp.bfloat16), "tp", scatter_dimension=1, tiled=True
    ).astype(jnp.float32)
    return (mixed, next_state)


def shards(
    residual_in,
    gain_pre,
    gate_pre,
    up_pre,
    down_pre,
    gain_mix,
    query_weight,
    forget_weight,
    value_weight,
    outgate_weight,
    lower_bound,
    head_gain,
    out_weight,
    gain_post,
    gate_post,
    up_post,
    down_post,
    memory_state,
):
    branch_a = channel_mixer(residual_in, gain_pre, gate_pre, up_pre, down_pre)
    stream_a = (residual_in.astype(jnp.float32) + 0.5 * branch_a).astype(jnp.bfloat16)
    mixed, next_state = token_mixer(
        stream_a,
        gain_mix,
        query_weight,
        forget_weight,
        value_weight,
        outgate_weight,
        lower_bound,
        head_gain,
        out_weight,
        memory_state,
    )
    stream_b = (stream_a.astype(jnp.float32) + mixed).astype(jnp.bfloat16)
    branch_b = channel_mixer(stream_b, gain_post, gate_post, up_post, down_post)
    layer_out = (stream_b.astype(jnp.float32) + 0.5 * branch_b).astype(jnp.bfloat16)
    return (layer_out, next_state)


ROW_PAD = 8
GATHER_A, SCATTER_A, COLUMNS, PROJECT, GATHER_B, SCATTER_B = 0, 1, 2, 3, 7, 8
KV_EXCHANGES = 9


def dot_columns(rows, weight_columns):
    return lax.dot_general(
        rows, weight_columns, (((1,), (1,)), ((), ())), preferred_element_type=jnp.float32
    )


def fused_layer(
    n_kv,
    residual_ref,
    gain_pre_ref,
    gain_mix_ref,
    lower_ref,
    head_gain_ref,
    gain_post_ref,
    gate_pre_hbm,
    up_pre_hbm,
    down_pre_hbm,
    query_hbm,
    forget_hbm,
    value_hbm,
    outgate_hbm,
    out_hbm,
    gate_post_hbm,
    up_post_hbm,
    down_post_hbm,
    state_hbm,
    layer_ref,
    next_hbm,
    gate_pre,
    up_pre,
    down_pre,
    proj_weights,
    out_weight,
    gate_post,
    up_post,
    down_post,
    state,
    gather_a,
    gather_b,
    partial_a,
    partial_b,
    landed_a,
    landed_b,
    gate_up_out,
    gate_up_in,
    squares_out,
    squares_in,
    stream_out,
    stream_in,
    column_out,
    column_in,
    proj_out,
    proj_in,
    mixed_out,
    mixed_in,
    residual_pad,
    sums_pad,
    keep_t,
    inject_t,
    query_t,
    value_rows,
    readout,
    load_sem,
    store_sem,
    kv_send,
    kv_recv,
    tp_send,
    tp_recv,
):
    me = lax.axis_index("kv")
    core = lax.axis_index("tp")
    rows, width = residual_ref.shape
    model = 2 * width
    f32, bf16 = jnp.float32, jnp.bfloat16

    def load(index, source, target):
        return pltpu.make_async_copy(source, target, load_sem.at[index])

    loads = [
        load(0, gate_pre_hbm, gate_pre),
        load(1, up_pre_hbm, up_pre),
        load(2, down_pre_hbm, down_pre),
        load(3, forget_hbm, proj_weights.at[0]),
        load(4, value_hbm, proj_weights.at[1]),
        load(5, query_hbm, proj_weights.at[2]),
        load(6, outgate_hbm, proj_weights.at[3]),
        load(7, state_hbm, state),
        load(8, out_hbm, out_weight),
        load(9, gate_post_hbm, gate_post),
        load(10, up_post_hbm, up_post),
        load(11, down_post_hbm, down_post),
    ]
    for copy in loads:
        copy.start()

    residual_pad[...] = jnp.zeros_like(residual_pad)
    residual_pad[0:rows, :] = residual_ref[...].astype(f32)
    gather_a[me] = residual_pad[...].astype(bf16)
    readout[...] = jnp.zeros_like(readout)
    sums_pad[...] = jnp.zeros_like(sums_pad)

    barrier = pltpu.get_barrier_semaphore()

    def greet(step, carry):
        pl.semaphore_signal(
            barrier,
            inc=1,
            device_id={"kv": lax.rem(me + step, n_kv)},
            device_id_type=pl.DeviceIdType.MESH,
        )
        return carry

    lax.fori_loop(1, n_kv, greet, 0)
    pl.semaphore_signal(
        barrier, inc=1, device_id={"tp": 1 - core}, device_id_type=pl.DeviceIdType.MESH
    )
    pl.semaphore_wait(barrier, n_kv)

    def kv_copy(exchange, source, target, peer, slot):
        return pltpu.make_async_remote_copy(
            src_ref=source,
            dst_ref=target,
            send_sem=kv_send.at[exchange, peer],
            recv_sem=kv_recv.at[exchange, slot],
            device_id={"kv": peer},
            device_id_type=pl.DeviceIdType.MESH,
        )

    def kv_start(exchange, source_of, target):
        def body(step, carry):
            peer = lax.rem(me + step, n_kv)
            kv_copy(exchange, source_of(peer), target.at[me], peer, me).start()
            return carry

        lax.fori_loop(1, n_kv, body, 0)

    def kv_arrive(exchange, target):
        def body(step, carry):
            peer = lax.rem(me + step, n_kv)
            kv_copy(exchange, target.at[peer], target.at[peer], peer, peer).wait_recv()
            return carry

        lax.fori_loop(1, n_kv, body, 0)

    def kv_sent(exchange, source_of, target):
        def body(step, carry):
            peer = lax.rem(me + step, n_kv)
            kv_copy(exchange, source_of(peer), target.at[me], peer, me).wait_send()
            return carry

        lax.fori_loop(1, n_kv, body, 0)

    def tp_copy(index, source, target):
        return pltpu.make_async_remote_copy(
            src_ref=source,
            dst_ref=target,
            send_sem=tp_send.at[index],
            recv_sem=tp_recv.at[index],
            device_id={"tp": 1 - core},
            device_id_type=pl.DeviceIdType.MESH,
        )

    def feed_forward(which, gathered, gain_ref, gate, up, down, partial, landed):
        gather_id, scatter_id = ((GATHER_A, SCATTER_A), (GATHER_B, SCATTER_B))[which]
        kv_start(gather_id, lambda peer: gathered.at[me], gathered)
        for copy in (loads[0:2], loads[9:11])[which]:
            copy.wait()
        kv_arrive(gather_id, gathered)
        wide = gathered[...].astype(f32).reshape(n_kv * ROW_PAD, width)
        squares = jnp.sum(wide * wide, axis=1, keepdims=True)
        squares_out[which] = jnp.broadcast_to(squares, squares_out.shape[1:])
        scaled = (wide * gain_ref[...]).astype(bf16)
        gate_part = dot_columns(scaled, gate[...])
        gate_up_out[which, 0] = gate_part.astype(bf16)
        copies = [
            tp_copy(3 * which, squares_out.at[which], squares_in.at[which]),
            tp_copy(3 * which + 1, gate_up_out.at[which, 0], gate_up_in.at[which, 0]),
            tp_copy(3 * which + 2, gate_up_out.at[which, 1], gate_up_in.at[which, 1]),
        ]
        copies[0].start()
        copies[1].start()
        up_part = dot_columns(scaled, up[...])
        gate_up_out[which, 1] = up_part.astype(bf16)
        copies[2].start()
        for copy in copies:
            copy.wait_recv()
        total = squares + squares_in[which][:, 0:1]
        inverse = lax.rsqrt(total / model + EPSILON)
        gate_sum = (gate_part + gate_up_in[which, 0].astype(f32)) * inverse
        up_sum = (up_part + gate_up_in[which, 1].astype(f32)) * inverse
        hidden = (gate_sum / (1.0 + jnp.exp(-gate_sum)) * up_sum).astype(bf16)
        loads[(2, 11)[which]].wait()
        branch = jnp.dot(hidden, down[...], preferred_element_type=f32)
        partial[...] = branch.reshape(n_kv, ROW_PAD, width)[:, 0:rows, :].astype(bf16)
        landed[me] = partial[me]
        kv_start(scatter_id, lambda peer: partial.at[peer], landed)
        kv_arrive(scatter_id, landed)
        for copy in copies:
            copy.wait_send()
        sums_pad[4 + which, 0:rows, :] = jnp.sum(landed[...].astype(f32), axis=0)
        return sums_pad[4 + which]

    branch_a = feed_forward(
        0, gather_a, gain_pre_ref, gate_pre, up_pre, down_pre, partial_a, landed_a
    )
    stream_a = (residual_pad[...] + 0.5 * branch_a).astype(bf16)

    stream_out[...] = stream_a
    stream_copy = tp_copy(6, stream_out, stream_in)
    stream_copy.start()
    own = stream_a.astype(f32)
    own_squares = jnp.sum(own * own, axis=1, keepdims=True)
    stream_copy.wait_recv()
    other = stream_in[...].astype(f32)
    squares = own_squares + jnp.sum(other * other, axis=1, keepdims=True)
    inverse = lax.rsqrt(squares / model + EPSILON)
    own_scaled = (own * gain_mix_ref[core]).astype(bf16)
    other_scaled = (other * gain_mix_ref[1 - core]).astype(bf16)
    depth = column_out.shape[2]
    half_blocks = n_kv // 2
    for block in range(half_blocks):
        span = slice(block * depth, (block + 1) * depth)
        column_out[core * half_blocks + block] = own_scaled[:, span]
        column_out[(1 - core) * half_blocks + block] = other_scaled[:, span]
    column_in[me] = column_out[me]
    kv_start(COLUMNS, lambda peer: column_out.at[peer], column_in)
    kv_arrive(COLUMNS, column_in)
    columns = column_in[...].astype(f32).reshape(n_kv * ROW_PAD, depth).astype(bf16)
    for index in range(4):
        loads[3 + index].wait()
        product = jnp.dot(columns, proj_weights[index], preferred_element_type=f32)
        proj_out[index] = product.reshape(n_kv, ROW_PAD, width)[:, 0:rows, :].astype(bf16)
        proj_in[index, me] = proj_out[index, me]
        kv_start(
            PROJECT + index,
            lambda peer, index=index: proj_out.at[index, peer],
            proj_in.at[index],
        )

    def projected(index):
        kv_arrive(PROJECT + index, proj_in.at[index])
        sums_pad[index, 0:rows, :] = jnp.sum(proj_in[index].astype(f32), axis=0)
        return sums_pad[index] * inverse

    heads = width // HEAD_DIM
    floor_rate = lower_ref[...]
    forget_pre = projected(0)
    keep = floor_rate + (1.0 - floor_rate) / (1.0 + jnp.exp(-forget_pre))
    inject = (1.0 - floor_rate) / (1.0 + jnp.exp(forget_pre))
    for head in range(heads):
        span = slice(head * HEAD_DIM, (head + 1) * HEAD_DIM)
        keep_t[head] = keep[:, span].T
        inject_t[head] = inject[:, span].T
    value_pre = projected(1)
    for head in range(heads):
        span = slice(head * HEAD_DIM, (head + 1) * HEAD_DIM)
        value_rows[head] = value_pre[:, span]
    query_pre = projected(2)
    query = query_pre / (1.0 + jnp.exp(-query_pre))
    for head in range(heads):
        span = slice(head * HEAD_DIM, (head + 1) * HEAD_DIM)
        query_t[head] = query[:, span].T
    loads[7].wait()

    def recur(head, carry):
        keep_cols = keep_t[head]
        inject_cols = inject_t[head]
        query_cols = query_t[head]
        values = value_rows[head]
        for row in range(rows):
            col = slice(row, row + 1)
            new = keep_cols[:, col] * state[row, head] + inject_cols[:, col] * values[col, :]
            state[row, head] = new
            readout[head, col, :] = jnp.sum(query_cols[:, col] * new, axis=0, keepdims=True)
        return carry

    lax.fori_loop(0, heads, recur, 0)
    store = pltpu.make_async_copy(state, next_hbm, store_sem)
    outgate_pre = projected(3)
    store.start()
    outgate = outgate_pre / (1.0 + jnp.exp(-outgate_pre))
    mixed_heads = []
    for head in range(heads):
        span = slice(head * HEAD_DIM, (head + 1) * HEAD_DIM)
        read = readout[head]
        scale = lax.rsqrt(jnp.mean(read * read, axis=1, keepdims=True) + EPSILON)
        mixed_heads.append(read * scale * head_gain_ref[:, span] * outgate[:, span])
    mixed_rows = jnp.concatenate(mixed_heads, axis=1).astype(bf16)
    loads[8].wait()
    mixed_part = jnp.dot(mixed_rows, out_weight[...], preferred_element_type=f32)
    mixed_out[0] = mixed_part[:, 0:width]
    mixed_out[1] = mixed_part[:, width:model]
    mixed_copy = tp_copy(7, mixed_out.at[1 - core], mixed_in)
    mixed_copy.start()
    mixed_copy.wait_recv()
    mixed = mixed_out[core] + mixed_in[...]
    stream_b = (stream_out[...].astype(f32) + mixed).astype(bf16)
    gather_b[me] = stream_b
    branch_b = feed_forward(
        1, gather_b, gain_post_ref, gate_post, up_post, down_post, partial_b, landed_b
    )
    layer_out = (gather_b[me].astype(f32) + 0.5 * branch_b).astype(bf16)
    layer_ref[...] = layer_out[0:rows, :]

    stream_copy.wait_send()
    mixed_copy.wait_send()
    kv_sent(GATHER_A, lambda peer: gather_a.at[me], gather_a)
    kv_sent(SCATTER_A, lambda peer: partial_a.at[peer], landed_a)
    kv_sent(COLUMNS, lambda peer: column_out.at[peer], column_in)
    for index in range(4):
        kv_sent(
            PROJECT + index,
            lambda peer, index=index: proj_out.at[index, peer],
            proj_in.at[index],
        )
    kv_sent(GATHER_B, lambda peer: gather_b.at[me], gather_b)
    kv_sent(SCATTER_B, lambda peer: partial_b.at[peer], landed_b)
    store.wait()


def fused_shards(
    n_kv,
    residual_in,
    gain_pre,
    gate_pre,
    up_pre,
    down_pre,
    gain_mix,
    query_weight,
    forget_weight,
    value_weight,
    outgate_weight,
    lower_bound,
    head_gain,
    out_weight,
    gain_post,
    gate_post,
    up_post,
    down_post,
    memory_state,
):
    rows, width = residual_in.shape
    depth = query_weight.shape[0]
    hidden = gate_pre.shape[1]
    heads = width // HEAD_DIM
    all_rows = n_kv * ROW_PAD
    f32, bf16 = jnp.float32, jnp.bfloat16
    vmem = pl.BlockSpec(memory_space=pltpu.VMEM)
    hbm = pl.BlockSpec(memory_space=pl.ANY)
    like = lambda array: pltpu.VMEM(array.shape, array.dtype)
    blocks = lambda count: pltpu.VMEM((n_kv, count, width), bf16)
    return pl.pallas_call(
        functools.partial(fused_layer, n_kv),
        out_shape=(
            jax.ShapeDtypeStruct(residual_in.shape, residual_in.dtype),
            jax.ShapeDtypeStruct(memory_state.shape, memory_state.dtype),
        ),
        in_specs=[vmem] * 6 + [hbm] * 12,
        out_specs=(vmem, hbm),
        scratch_shapes=[
            pltpu.VMEM((hidden, width), bf16),
            pltpu.VMEM((hidden, width), bf16),
            like(down_pre),
            pltpu.VMEM((4,) + query_weight.shape, bf16),
            like(out_weight),
            pltpu.VMEM((hidden, width), bf16),
            pltpu.VMEM((hidden, width), bf16),
            like(down_post),
            like(memory_state),
            blocks(ROW_PAD),
            blocks(ROW_PAD),
            blocks(rows),
            blocks(rows),
            blocks(rows),
            blocks(rows),
            pltpu.VMEM((2, 2, all_rows, hidden), bf16),
            pltpu.VMEM((2, 2, all_rows, hidden), bf16),
            pltpu.VMEM((2, all_rows, 128), f32),
            pltpu.VMEM((2, all_rows, 128), f32),
            pltpu.VMEM((ROW_PAD, width), bf16),
            pltpu.VMEM((ROW_PAD, width), bf16),
            pltpu.VMEM((n_kv, ROW_PAD, depth), bf16),
            pltpu.VMEM((n_kv, ROW_PAD, depth), bf16),
            pltpu.VMEM((4, n_kv, rows, width), bf16),
            pltpu.VMEM((4, n_kv, rows, width), bf16),
            pltpu.VMEM((2, ROW_PAD, width), f32),
            pltpu.VMEM((ROW_PAD, width), f32),
            pltpu.VMEM((ROW_PAD, width), f32),
            pltpu.VMEM((6, ROW_PAD, width), f32),
            pltpu.VMEM((heads, HEAD_DIM, ROW_PAD), f32),
            pltpu.VMEM((heads, HEAD_DIM, ROW_PAD), f32),
            pltpu.VMEM((heads, HEAD_DIM, ROW_PAD), f32),
            pltpu.VMEM((heads, ROW_PAD, HEAD_DIM), f32),
            pltpu.VMEM((heads, ROW_PAD, HEAD_DIM), f32),
            pltpu.SemaphoreType.DMA((12,)),
            pltpu.SemaphoreType.DMA,
            pltpu.SemaphoreType.DMA((KV_EXCHANGES, n_kv)),
            pltpu.SemaphoreType.DMA((KV_EXCHANGES, n_kv)),
            pltpu.SemaphoreType.DMA((8,)),
            pltpu.SemaphoreType.DMA((8,)),
        ],
        compiler_params=pltpu.CompilerParams(
            collective_id=0, has_side_effects=True, vmem_limit_bytes=60 * 1024 * 1024
        ),
    )(
        residual_in,
        gain_pre.reshape(1, width),
        gain_mix.reshape(2, 1, width),
        lower_bound.reshape(1, width),
        head_gain.reshape(1, width),
        gain_post.reshape(1, width),
        gate_pre.T,
        up_pre.T,
        down_pre,
        query_weight,
        forget_weight,
        value_weight,
        outgate_weight,
        out_weight,
        gate_post.T,
        up_post.T,
        down_post,
        memory_state,
    )


def solution(mesh):
    n_kv, n_tp = mesh.shape["kv"], mesh.shape["tp"]
    fits = n_tp == 2 and D % (128 * n_kv) == 0 and n_kv % 2 == 0
    body = functools.partial(fused_shards, n_kv) if fits else shards
    in_specs = (
        P("kv", "tp"),
        P("tp"),
        P("tp", "kv"),
        P("tp", "kv"),
        P("kv", "tp"),
        P(),
        P("kv", "tp"),
        P("kv", "tp"),
        P("kv", "tp"),
        P("kv", "tp"),
        P("tp"),
        P("tp"),
        P("tp", None),
        P("tp"),
        P("tp", "kv"),
        P("tp", "kv"),
        P("kv", "tp"),
        P("kv", "tp", None, None),
    )
    out_specs = (P("kv", "tp"), P("kv", "tp", None, None))
    return jax.shard_map(body, mesh=mesh, in_specs=in_specs, out_specs=out_specs, check_vma=False)
```
